32 devices in a mesh: sp: 8 (over z, y), tp: 4 (over x, core).
Axes of the slice: x: 2, y: 2, z: 4, core: 2. Of those that a mesh axis runs over, the one named last changes fastest.
Arguments:
- queries: bfloat16 [3072, 2048], P('sp', 'tp'), may hold values from -6 to 6
- keys: bfloat16 [3072, 2048], P('sp', 'tp'), may hold values from -6 to 6
- values: bfloat16 [3072, 2048], P('sp', 'tp'), may hold values from -6 to 6
- gates: bfloat16 [3072, 2048], P('sp', 'tp'), may hold values from -8 to 8
- decay_pre: float32 [32, 3072], P('tp', 'sp'), may hold values from -18 to 3
- beta_pre: float32 [32, 3072], P('tp', 'sp'), may hold values from -10 to 3
- out_gain: float32 [64], replicated, may hold values from 0.1 to 1.9
- w_out: bfloat16 [2048, 2048], P('tp'), may hold values from -0.125 to 0.125
- stream: bfloat16 [3072, 2048], P(('sp', 'tp')), may hold values from -6 to 6
- norm_gain: float32 [2048], replicated, may hold values from 0.1 to 1.9
- w_gate: bfloat16 [2048, 5632], P('sp', 'tp'), may hold values from -0.125 to 0.125
- w_up: bfloat16 [2048, 5632], P('sp', 'tp'), may hold values from -0.125 to 0.125
- w_down: bfloat16 [5632, 2048], P('tp', 'sp'), may hold values from -0.078125 to 0.078125
Outputs:
- updated: bfloat16 [3072, 2048], P(('sp', 'tp'))
The draws below stay inside these ranges and needn't reach their ends.
All inputs are finite; a program needn't handle non-finite values.
Results may differ from the reference program's by a relative error of at most 0.019.
Values may be sent and summed in bfloat16 or wider, within the bound.
A program may use at most 128 MiB of HBM per device.

```python
import math
import jax
import jax.numpy as jnp
from jax import lax

D = 2048
HEADS = 32
HEAD_DIM = 64
FF = 5632
BLOCK = 64
TOK_DEV = 384
TOKEN_POSITIONS = 3072
N_TP = 4


def slow_heads(key):
    order = jax.random.permutation(jax.random.fold_in(key, 17), HEADS)
    keep_count = HEADS // 2
    return order < keep_count


def draw_decay_pre(key, part):
    slow = slow_heads(key)[:, None]
    noise_random_key, shard_random_key, spike_random_key = jax.random.split(jax.random.fold_in(key, 29), 3)
    small_noise = jnp.clip(jax.random.normal(noise_random_key, (HEADS, TOKEN_POSITIONS), jnp.float32), -3.0, 3.0)
    span_levels = jax.random.uniform(shard_random_key, (HEADS, TOKEN_POSITIONS // TOK_DEV), jnp.float32, -0.7, 0.7)
    noise_deviation = jnp.repeat(span_levels, TOK_DEV, axis=1)
    slow_level = math.log(0.35 / TOKEN_POSITIONS) - 0.5
    fast_level = math.log(0.04) - 0.5
    noise_amplitude = jnp.where(slow, slow_level, fast_level)
    spike_locations = jax.random.randint(spike_random_key, (3,), 0, TOKEN_POSITIONS)
    token_places = jnp.arange(TOKEN_POSITIONS)
    spike_mask = jnp.any(token_places[None, :] == spike_locations[:, None], axis=0)
    return jnp.where(spike_mask[None, :], -1.0, noise_amplitude + small_noise + noise_deviation).astype(jnp.float32)


def draw_beta_pre(key, part):
    slow = slow_heads(key)[:, None]
    noise_random_key = jax.random.fold_in(key, 43)
    small_noise = jnp.clip(0.6 * jax.random.normal(noise_random_key, (HEADS, TOKEN_POSITIONS), jnp.float32), -3.0, 3.0)
    rate = min(82.0 / TOKEN_POSITIONS, 0.5)
    slow_level = math.log(rate / (1.0 - rate))
    return (jnp.where(slow, slow_level, 0.0) + small_noise).astype(jnp.float32)


def shard_levels(stream_key, dims, cuts, least, largest):
    def one(position, blocks):
        heights = jax.random.uniform(jax.random.fold_in(jax.random.fold_in(stream_key, 6), position), (blocks,), jnp.float32, least / len(cuts), largest / len(cuts))
        return jnp.repeat(jnp.exp(heights), dims[position] // blocks).reshape((-1,) + (1,) * (len(dims) - position - 1))

    level = one(*cuts[0])
    for cut in cuts[1:]:
        level = level * one(*cut)
    return level


def centred(own_key, shape, spread, bound, shards=(), kind=jnp.bfloat16):
    values = jax.random.normal(own_key, shape, jnp.float32) * spread
    if len(shards) > 0:
        values = shard_levels(own_key, shape, shards, -0.22, 0.18) * values
    return jnp.clip(values, min=-bound, max=bound).astype(kind)


def setup_inputs(seed: int = 0) -> dict:
    key_of = jax.random.split(jax.random.key(seed), 14)
    return {
        "queries": centred(key_of[0], (TOKEN_POSITIONS, HEADS * HEAD_DIM), 1.0, 6.0, ((0, 8), (1, 4))),
        "keys": centred(key_of[1], (TOKEN_POSITIONS, HEADS * HEAD_DIM), 1.0, 6.0, ((0, 8), (1, 4))),
        "values": centred(key_of[2], (TOKEN_POSITIONS, HEADS * HEAD_DIM), 1.0, 6.0, ((0, 8), (1, 4))),
        "gates": centred(key_of[3], (TOKEN_POSITIONS, HEADS * HEAD_DIM), 1.5, 8.0, ((0, 8), (1, 4))),
        "decay_pre": draw_decay_pre(jax.random.fold_in(key_of[13], 71), 0),
        "beta_pre": draw_beta_pre(jax.random.fold_in(key_of[13], 71), 0),
        "out_gain": jnp.clip(1.0 + 0.18 * jax.random.normal(key_of[6], (HEAD_DIM,), jnp.float32), 0.1, 1.9),
        "w_out": centred(key_of[7], (HEADS * HEAD_DIM, D), (HEADS * HEAD_DIM) ** -0.5, 0.125, ((0, 4),)),
        "stream": centred(key_of[8], (TOKEN_POSITIONS, D), 1.0, 6.0, ((0, 32),)),
        "norm_gain": jnp.clip(1.0 + 0.18 * jax.random.normal(key_of[9], (D,), jnp.float32), 0.1, 1.9),
        "w_gate": centred(key_of[10], (D, FF), D ** -0.5, 0.125, ((0, 8), (1, 4))),
        "w_up": centred(key_of[11], (D, FF), D ** -0.5, 0.125, ((0, 8), (1, 4))),
        "w_down": centred(key_of[12], (FF, D), FF ** -0.5, 0.078125, ((0, 4), (1, 8))),
    }


EPSILON = 1e-06
EXACT_PRECISION = lax.Precision.HIGHEST

def unit_lower_inverse(lower_mat):
    span_len = lower_mat.shape[-1]
    identity = jnp.eye(span_len, dtype=jnp.float32)
    power = -lower_mat
    inverse = identity + power
    steps = 1
    while 1 << steps < span_len:
        power = jnp.einsum('...ij,...jk->...ik', power, power, precision=EXACT_PRECISION)
        inverse = jnp.einsum('...ij,...jk->...ik', inverse, identity + power, precision=EXACT_PRECISION)
        steps = steps + 1
    return inverse

def prepare(queries, keys, values, beta_pre, decay_pre):
    length = queries.shape[0]
    heads = queries.shape[1] // HEAD_DIM

    def split_heads(arr):
        return arr.astype(jnp.float32).reshape(length, heads, HEAD_DIM)
    query_unit = jax.nn.silu(split_heads(queries))
    query_unit = query_unit * lax.rsqrt(lax.optimization_barrier(jnp.sum(query_unit * query_unit, axis=-1, keepdims=True)) + EPSILON)
    query_unit = (query_unit * HEAD_DIM ** (-0.5)).astype(jnp.bfloat16)
    key_unit = jax.nn.silu(split_heads(keys))
    key_unit = (key_unit * lax.rsqrt(lax.optimization_barrier(jnp.sum(key_unit * key_unit, axis=-1, keepdims=True)) + EPSILON)).astype(jnp.bfloat16)
    value_act = jax.nn.silu(split_heads(values))
    strength = jax.nn.sigmoid(beta_pre.astype(jnp.float32))
    log_decay = -jax.nn.softplus(decay_pre.astype(jnp.float32))
    nblocks = length // BLOCK

    def blocked(arr):
        return arr.reshape(nblocks, BLOCK, heads, HEAD_DIM).transpose(0, 2, 1, 3)

    def blocked_rates(arr):
        return arr.reshape(heads, nblocks, BLOCK).transpose(1, 0, 2)
    return (blocked(query_unit), blocked(key_unit), blocked(value_act), blocked_rates(strength), blocked_rates(log_decay))

def block_terms(query_blk, key_blk, value_blk, strength_blk, decay_blk):
    span_len = query_blk.shape[-2]
    query_f = query_blk.astype(jnp.float32)
    key_f = key_blk.astype(jnp.float32)
    cumulative = jnp.cumsum(decay_blk, axis=-1)
    row_ids = jnp.arange(span_len)[:, None]
    col_ids = jnp.arange(span_len)[None, :]
    inclusive = row_ids >= col_ids
    strict = row_ids > col_ids
    decay_mat = jnp.exp(jnp.where(inclusive, cumulative[..., :, None] - cumulative[..., None, :], -jnp.inf))
    key_inner = jnp.einsum('...id,...jd->...ij', key_f, key_f, precision=EXACT_PRECISION)
    lower_mat = jnp.where(strict, strength_blk[..., :, None] * key_inner * decay_mat, 0.0)
    key_strong = key_f * strength_blk[..., None]
    right_side = jnp.concatenate([value_blk * strength_blk[..., None], key_strong * jnp.exp(cumulative)[..., None]], axis=-1)
    solved = jnp.einsum('...ij,...jk->...ik', unit_lower_inverse(lower_mat), right_side, precision=EXACT_PRECISION)
    width = value_blk.shape[-1]
    update_values = solved[..., :width]
    update_keys = solved[..., width:]
    query_inner = jnp.einsum('...id,...jd->...ij', query_f, key_f, precision=EXACT_PRECISION)
    inside_span = jnp.where(inclusive, query_inner * decay_mat, 0.0)
    final_decay = cumulative[..., -1:]
    key_attenuated = key_f * jnp.exp(final_decay - cumulative)[..., None]
    query_attenuated = query_f * jnp.exp(cumulative)[..., None]
    return (update_values, update_keys, inside_span, query_attenuated, key_attenuated, final_decay)

def advance(matrix_state, terms):
    update_values, update_keys, inside_span, query_attenuated, key_attenuated, final_decay = terms
    value_corrected = update_values - jnp.einsum('jod,jdg->jog', update_keys, matrix_state, precision=EXACT_PRECISION)
    output_result = jnp.einsum('jod,jdg->jog', query_attenuated, matrix_state, precision=EXACT_PRECISION) + jnp.einsum('oyn,onk->oyk', inside_span, value_corrected, precision=EXACT_PRECISION)
    matrix_state = matrix_state * jnp.exp(final_decay)[..., None] + jnp.einsum('lyq,lyf->lqf', key_attenuated, value_corrected, precision=EXACT_PRECISION)
    return (matrix_state, output_result)

def finish(outputs, gates, out_gain):
    length = gates.shape[0]
    heads = gates.shape[1] // HEAD_DIM
    heads_out = outputs.transpose(0, 2, 1, 3).reshape(length, heads, HEAD_DIM)
    heads_out = heads_out * lax.rsqrt(lax.optimization_barrier(jnp.mean(heads_out * heads_out, axis=-1, keepdims=True)) + EPSILON)
    heads_out = heads_out * out_gain.astype(jnp.float32)
    gated = heads_out * jax.nn.silu(gates.astype(jnp.float32).reshape(length, heads, HEAD_DIM))
    return gated.reshape(length, heads * HEAD_DIM).astype(jnp.bfloat16)

def reference(queries, keys, values, gates, decay_pre, beta_pre, out_gain, w_out, stream, norm_gain, w_gate, w_up, w_down):
    blocks = prepare(queries, keys, values, beta_pre, decay_pre)
    terms = block_terms(*blocks)
    heads = queries.shape[1] // HEAD_DIM
    start_state = jnp.zeros((heads, HEAD_DIM, HEAD_DIM), jnp.float32)
    _, outputs = lax.scan(advance, start_state, terms)
    mixed_heads = finish(outputs, gates, out_gain)
    projected = jnp.dot(mixed_heads, w_out, preferred_element_type=jnp.float32)
    middle = (stream.astype(jnp.float32) + projected).astype(jnp.bfloat16)
    middle_f = middle.astype(jnp.float32)
    normed = middle_f * lax.rsqrt(lax.optimization_barrier(jnp.mean(middle_f * middle_f, axis=-1, keepdims=True)) + EPSILON)
    normed = (normed * norm_gain.astype(jnp.float32)).astype(jnp.bfloat16)
    length = normed.shape[0]
    group_width = FF // N_TP

    def ffn_block(rows):
        gate_hidden = jnp.dot(rows, w_gate, preferred_element_type=jnp.float32)
        up_hidden = jnp.dot(rows, w_up, preferred_element_type=jnp.float32)
        hidden = (jax.nn.silu(gate_hidden) * up_hidden).astype(jnp.bfloat16)
        total = jnp.zeros((rows.shape[0], w_down.shape[1]), jnp.float32)
        for member in range(N_TP):
            partial_sum = jnp.dot(hidden[:, member * group_width:(member + 1) * group_width], w_down[member * group_width:(member + 1) * group_width], preferred_element_type=jnp.float32).astype(jnp.bfloat16)
            partial_sum = lax.optimization_barrier(partial_sum)
            total = total + partial_sum.astype(jnp.float32)
        return total
    row_blocks = normed.reshape(length // TOK_DEV, TOK_DEV, normed.shape[1])
    channel_sum = lax.map(ffn_block, row_blocks).reshape(length, normed.shape[1])
    return (middle_f + 0.5 * channel_sum).astype(jnp.bfloat16)
```

```python
import functools

import jax
import jax.numpy as jnp
from jax import lax
from jax.experimental import pallas as pl
from jax.experimental.pallas import tpu as pltpu
from jax.sharding import PartitionSpec as P

HEAD_DIM = 64
EPSILON = 1e-06
EXACT_PRECISION = lax.Precision.HIGHEST
CHUNK = 128
PAIR = 2 * HEAD_DIM


def split_dot(left, right, dims):
    high = left.astype(jnp.bfloat16)
    low = (left - high.astype(jnp.float32)).astype(jnp.bfloat16)
    return dot(high, right, dims) + dot(low, right, dims)


def dot(left, right, dims):
    return lax.dot_general(
        left.astype(jnp.bfloat16),
        right.astype(jnp.bfloat16),
        (dims, ((), ())),
        preferred_element_type=jnp.float32,
    )


NN = ((1,), (0,))
NT = ((1,), (1,))
TN = ((0,), (0,))


def exact_dot(left, right, dims):
    return lax.dot_general(
        left, right, (dims, ((), ())), precision=EXACT_PRECISION, preferred_element_type=jnp.float32
    )


def silu(x):
    return x / (1.0 + jnp.exp(-x))


def iotas(rows, columns):
    return (
        lax.broadcasted_iota(jnp.int32, (rows, columns), 0),
        lax.broadcasted_iota(jnp.int32, (rows, columns), 1),
    )


def lower_inverse(lower, row_ids, col_ids):
    small = 16
    near = jnp.where(row_ids // small == col_ids // small, lower, 0.0)
    power = -near
    rest = power
    size = 2
    while size < small:
        power = dot(power, power, NN)
        rest = rest + power + dot(rest, power, NN)
        size *= 2
    size = small
    while size < lower.shape[0]:
        off = jnp.where(
            (row_ids // (2 * size) == col_ids // (2 * size)) & (row_ids // size != col_ids // size),
            lower,
            0.0,
        )
        half = off + dot(off, rest, NN)
        rest = rest - half - dot(rest, half, NN)
        size *= 2
    return rest


def mixer_kernel(q_ref, k_ref, v_ref, beta_ref, decay_ref, state_ref, local_ref, reach_ref):
    length, width = q_ref.shape
    pairs = width // PAIR
    row_ids, col_ids = iotas(CHUNK, CHUNK)
    inclusive = row_ids >= col_ids
    strict = row_ids > col_ids
    eye = (row_ids == col_ids).astype(jnp.float32)
    lower_ones = inclusive.astype(jnp.float32)
    same_half = (row_ids // HEAD_DIM == col_ids // HEAD_DIM).astype(jnp.bfloat16)
    first = col_ids < HEAD_DIM
    own = (first, jnp.logical_not(first))
    states = [
        [jnp.where(row_ids // HEAD_DIM == 1 - side, eye, 0.0) for side in range(2)]
        for _ in range(pairs)
    ]
    for chunk in range(length // CHUNK):
        rows = pl.ds(chunk * CHUNK, CHUNK)
        log_decay = -jax.nn.softplus(decay_ref[:, rows])
        strength = jax.nn.sigmoid(beta_ref[:, rows])
        cum_col = exact_dot(lower_ones, log_decay, NT)
        cum_row = exact_dot(log_decay, lower_ones, NT)
        strength_col = exact_dot(eye, strength, NT)
        grow_col = jnp.exp(cum_col)
        final_row = cum_col[CHUNK - 1 : CHUNK, :]
        fade_col = jnp.exp(final_row - cum_col)
        final_exp = jnp.exp(final_row)
        for pair in range(pairs):
            lanes = pl.ds(pair * PAIR, PAIR)

            def unit(ref):
                x = silu(ref[rows, lanes].astype(jnp.float32))
                total = split_dot(x * x, same_half, NN)
                return x * lax.rsqrt(total + EPSILON)

            query = (unit(q_ref) * HEAD_DIM ** (-0.5)).astype(jnp.bfloat16)
            key = unit(k_ref).astype(jnp.bfloat16)
            value = silu(v_ref[rows, lanes].astype(jnp.float32))
            query_turned = pltpu.roll(query.astype(jnp.float32), HEAD_DIM, 1)
            key_turned = pltpu.roll(key.astype(jnp.float32), HEAD_DIM, 1)
            outs = []
            for side in range(2):
                head = 2 * pair + side
                mine = own[side]
                col = slice(head, head + 1)
                cum = cum_col[:, col]
                decay_mat = jnp.exp(
                    jnp.where(inclusive, cum - cum_row[head : head + 1, :], -1e30)
                )
                masked = jnp.where(mine, key, jnp.zeros_like(key))
                key_inner = dot(masked, key, NT)
                query_inner = dot(query, masked, NT)
                lower = jnp.where(strict, strength_col[:, col] * key_inner * decay_mat, 0.0)
                right_side = strength_col[:, col] * jnp.where(
                    mine, value, key_turned * grow_col[:, col]
                )
                rest = lower_inverse(lower, row_ids, col_ids)
                solved = right_side + dot(rest, right_side, NN)
                state = states[pair][side]
                corrected = jnp.where(mine, solved, 0.0) - dot(
                    jnp.where(mine, 0.0, solved), state, NN
                )
                inside = query_inner * decay_mat
                result = dot(query_turned * grow_col[:, col], state, NN) + dot(
                    inside, corrected, NN
                )
                key_fading = jnp.where(mine, 0.0, key_turned * fade_col[:, col])
                states[pair][side] = state * final_exp[:, col] + dot(key_fading, corrected, TN)
                outs.append(result)
            local_ref[rows, lanes] = jnp.where(first, outs[0], outs[1])
            reach_ref[rows, lanes] = jnp.where(first, outs[1], outs[0]).astype(jnp.bfloat16)
    for pair in range(pairs):
        state_ref[pair] = (states[pair][0] + states[pair][1]).astype(jnp.bfloat16)


def mixer(queries, keys, values, beta_pre, decay_pre):
    length, width = queries.shape
    pairs = width // PAIR
    return pl.pallas_call(
        mixer_kernel,
        name="mixer",
        out_shape=(
            jax.ShapeDtypeStruct((pairs, PAIR, PAIR), jnp.bfloat16),
            jax.ShapeDtypeStruct((length, width), jnp.float32),
            jax.ShapeDtypeStruct((length, width), jnp.bfloat16),
        ),
        in_specs=[pl.BlockSpec(memory_space=pltpu.VMEM)] * 5,
        out_specs=(pl.BlockSpec(memory_space=pltpu.VMEM),) * 3,
        cost_estimate=pl.CostEstimate(
            flops=60 * length * PAIR * PAIR * pairs, bytes_accessed=8 * length * width, transcendentals=0
        ),
    )(queries, keys, values, beta_pre, decay_pre)


def finish_kernel(size, every_ref, local_ref, reach_ref, gates_ref, gain_ref, out_ref):
    length, width = local_ref.shape
    pairs = width // PAIR
    index = lax.axis_index("sp")
    row_ids, col_ids = iotas(PAIR, PAIR)
    same = row_ids // HEAD_DIM == col_ids // HEAD_DIM
    same_half = same.astype(jnp.bfloat16)

    def hop(step, before):
        reached = step < index
        after = []
        for pair in range(pairs):
            item = every_ref[step, pair]
            trans = jnp.where(same, item, jnp.zeros_like(item))
            offset = jnp.where(same, 0.0, item.astype(jnp.float32))
            high = before[pair].astype(jnp.bfloat16)
            low = (before[pair] - high.astype(jnp.float32)).astype(jnp.bfloat16)
            new = offset + dot(trans, high, NN) + dot(trans, low, NN)
            after.append(jnp.where(reached, new, before[pair]))
        return tuple(after)

    start = tuple(jnp.zeros((PAIR, PAIR), jnp.float32) for _ in range(pairs))
    earlier = lax.fori_loop(0, size - 1, hop, start)
    for pair in range(pairs):
        lanes = pl.ds(pair * PAIR, PAIR)
        heads_out = local_ref[:, lanes] + dot(reach_ref[:, lanes], earlier[pair], NN)
        mean = split_dot(heads_out * heads_out, same_half, NN) * (1.0 / HEAD_DIM)
        heads_out = heads_out * lax.rsqrt(mean + EPSILON) * gain_ref[...]
        gated = heads_out * silu(gates_ref[:, lanes].astype(jnp.float32))
        out_ref[:, lanes] = gated.astype(jnp.bfloat16)


def finish(every, local, reach, gates, out_gain):
    length, width = local.shape
    return pl.pallas_call(
        functools.partial(finish_kernel, every.shape[0]),
        name="finish",
        out_shape=jax.ShapeDtypeStruct((length, width), jnp.bfloat16),
        in_specs=[pl.BlockSpec(memory_space=pltpu.VMEM)] * 5,
        out_specs=pl.BlockSpec(memory_space=pltpu.VMEM),
        cost_estimate=pl.CostEstimate(
            flops=4 * length * width * PAIR, bytes_accessed=8 * length * width, transcendentals=0
        ),
    )(every, local, reach, gates, jnp.concatenate([out_gain, out_gain])[None, :])


def per_device(
    queries,
    keys,
    values,
    gates,
    decay_pre,
    beta_pre,
    out_gain,
    w_out,
    stream,
    norm_gain,
    w_gate,
    w_up,
    w_down,
):
    state, local, reach = mixer(queries, keys, values, beta_pre, decay_pre)
    every = lax.all_gather(state, "sp")
    mixed_heads = finish(every, local, reach, gates, out_gain)
    head_block = lax.all_to_all(mixed_heads, "tp", split_axis=0, concat_axis=1, tiled=True)
    out_whole = lax.all_gather(w_out, "tp", axis=0, tiled=True)
    projected = jnp.dot(head_block, out_whole, preferred_element_type=jnp.float32)
    middle = (stream.astype(jnp.float32) + projected).astype(jnp.bfloat16)
    middle_f = middle.astype(jnp.float32)
    normed = middle_f * lax.rsqrt(jnp.mean(middle_f * middle_f, axis=-1, keepdims=True) + EPSILON)
    normed = (normed * norm_gain).astype(jnp.bfloat16)
    span_rows = lax.all_gather(normed, "tp", axis=0, tiled=True)
    gate_hidden = jnp.dot(
        span_rows,
        lax.all_gather(w_gate, "sp", axis=0, tiled=True),
        preferred_element_type=jnp.float32,
    )
    up_hidden = jnp.dot(
        span_rows,
        lax.all_gather(w_up, "sp", axis=0, tiled=True),
        preferred_element_type=jnp.float32,
    )
    hidden = (jax.nn.silu(gate_hidden) * up_hidden).astype(jnp.bfloat16)
    channel_term = jnp.dot(
        hidden, lax.all_gather(w_down, "sp", axis=1, tiled=True), preferred_element_type=jnp.float32
    )
    channel_sum = lax.psum_scatter(
        channel_term.astype(jnp.bfloat16), "tp", scatter_dimension=0, tiled=True
    ).astype(jnp.float32)
    return (middle_f + 0.5 * channel_sum).astype(jnp.bfloat16)


def solution(mesh):
    return jax.shard_map(
        per_device,
        mesh=mesh,
        in_specs=(
            P("sp", "tp"),
            P("sp", "tp"),
            P("sp", "tp"),
            P("sp", "tp"),
            P("tp", "sp"),
            P("tp", "sp"),
            P(),
            P("tp", None),
            P(("sp", "tp"), None),
            P(),
            P("sp", "tp"),
            P("sp", "tp"),
            P("tp", "sp"),
        ),
        out_specs=P(("sp", "tp"), None),
        check_vma=False,
    )
```

```python
import functools

import jax
import jax.numpy as jnp
from jax import lax
from jax.experimental import pallas as pl
from jax.experimental.pallas import tpu as pltpu
from jax.sharding import PartitionSpec as P


HEAD_DIM = 64
EPSILON = 1e-06
EXACT_PRECISION = lax.Precision.HIGHEST
CHUNK = 128
PAIR = 2 * HEAD_DIM


def split_dot(left, right, dims):
    high = left.astype(jnp.bfloat16)
    low = (left - high.astype(jnp.float32)).astype(jnp.bfloat16)
    return dot(high, right, dims) + dot(low, right, dims)


def dot(left, right, dims):
    return lax.dot_general(
        left.astype(jnp.bfloat16),
        right.astype(jnp.bfloat16),
        (dims, ((), ())),
        preferred_element_type=jnp.float32,
    )


NN = ((1,), (0,))
NT = ((1,), (1,))
TN = ((0,), (0,))


def exact_dot(left, right, dims):
    return lax.dot_general(
        left, right, (dims, ((), ())), precision=EXACT_PRECISION, preferred_element_type=jnp.float32
    )


def silu(x):
    return x / (1.0 + jnp.exp(-x))


def iotas(rows, columns):
    return (
        lax.broadcasted_iota(jnp.int32, (rows, columns), 0),
        lax.broadcasted_iota(jnp.int32, (rows, columns), 1),
    )


def lower_inverse(lower, row_ids, col_ids):
    small = 16
    near = jnp.where(row_ids // small == col_ids // small, lower, 0.0)
    power = -near
    rest = power
    size = 2
    while size < small:
        power = dot(power, power, NN)
        rest = rest + power + dot(rest, power, NN)
        size *= 2
    size = small
    while size < lower.shape[0]:
        off = jnp.where(
            (row_ids // (2 * size) == col_ids // (2 * size)) & (row_ids // size != col_ids // size),
            lower,
            0.0,
        )
        half = off + dot(off, rest, NN)
        rest = rest - half - dot(rest, half, NN)
        size *= 2
    return rest


def mixer_kernel(q_ref, k_ref, v_ref, beta_ref, decay_ref, state_ref, local_ref, reach_ref):
    length, width = q_ref.shape
    pairs = width // PAIR
    row_ids, col_ids = iotas(CHUNK, CHUNK)
    inclusive = row_ids >= col_ids
    strict = row_ids > col_ids
    eye = (row_ids == col_ids).astype(jnp.float32)
    lower_ones = inclusive.astype(jnp.float32)
    same_half = (row_ids // HEAD_DIM == col_ids // HEAD_DIM).astype(jnp.bfloat16)
    first = col_ids < HEAD_DIM
    own = (first, jnp.logical_not(first))
    states = [
        [jnp.where(row_ids // HEAD_DIM == 1 - side, eye, 0.0) for side in range(2)]
        for _ in range(pairs)
    ]
    for chunk in range(length // CHUNK):
        rows = pl.ds(chunk * CHUNK, CHUNK)
        log_decay = -jax.nn.softplus(decay_ref[:, rows])
        strength = jax.nn.sigmoid(beta_ref[:, rows])
        cum_col = exact_dot(lower_ones, log_decay, NT)
        cum_row = exact_dot(log_decay, lower_ones, NT)
        strength_col = exact_dot(eye, strength, NT)
        grow_col = jnp.exp(cum_col)
        final_row = cum_col[CHUNK - 1 : CHUNK, :]
        fade_col = jnp.exp(final_row - cum_col)
        final_exp = jnp.exp(final_row)
        for pair in range(pairs):
            lanes = pl.ds(pair * PAIR, PAIR)

            def unit(ref):
                x = silu(ref[rows, lanes].astype(jnp.float32))
                total = split_dot(x * x, same_half, NN)
                return x * lax.rsqrt(total + EPSILON)

            query = (unit(q_ref) * HEAD_DIM ** (-0.5)).astype(jnp.bfloat16)
            key = unit(k_ref).astype(jnp.bfloat16)
            value = silu(v_ref[rows, lanes].astype(jnp.float32))
            query_turned = pltpu.roll(query.astype(jnp.float32), HEAD_DIM, 1)
            key_turned = pltpu.roll(key.astype(jnp.float32), HEAD_DIM, 1)
            outs = []
            for side in range(2):
                head = 2 * pair + side
                mine = own[side]
                col = slice(head, head + 1)
                cum = cum_col[:, col]
                decay_mat = jnp.exp(
                    jnp.where(inclusive, cum - cum_row[head : head + 1, :], -1e30)
                )
                masked = jnp.where(mine, key, jnp.zeros_like(key))
                key_inner = dot(masked, key, NT)
                query_inner = dot(query, masked, NT)
                lower = jnp.where(strict, strength_col[:, col] * key_inner * decay_mat, 0.0)
                right_side = strength_col[:, col] * jnp.where(
                    mine, value, key_turned * grow_col[:, col]
                )
                rest = lower_inverse(lower, row_ids, col_ids)
                solved = right_side + dot(rest, right_side, NN)
                state = states[pair][side]
                corrected = jnp.where(mine, solved, 0.0) - dot(
                    jnp.where(mine, 0.0, solved), state, NN
                )
                inside = query_inner * decay_mat
                result = dot(query_turned * grow_col[:, col], state, NN) + dot(
                    inside, corrected, NN
                )
                key_fading = jnp.where(mine, 0.0, key_turned * fade_col[:, col])
                states[pair][side] = state * final_exp[:, col] + dot(key_fading, corrected, TN)
                outs.append(result)
            local_ref[rows, lanes] = jnp.where(first, outs[0], outs[1])
            reach_ref[rows, lanes] = jnp.where(first, outs[1], outs[0]).astype(jnp.bfloat16)
    for pair in range(pairs):
        state_ref[pair] = (states[pair][0] + states[pair][1]).astype(jnp.bfloat16)


def mixer(queries, keys, values, beta_pre, decay_pre):
    length, width = queries.shape
    pairs = width // PAIR
    return pl.pallas_call(
        mixer_kernel,
        name="mixer",
        out_shape=(
            jax.ShapeDtypeStruct((pairs, PAIR, PAIR), jnp.bfloat16),
            jax.ShapeDtypeStruct((length, width), jnp.float32),
            jax.ShapeDtypeStruct((length, width), jnp.bfloat16),
        ),
        in_specs=[pl.BlockSpec(memory_space=pltpu.VMEM)] * 5,
        out_specs=(pl.BlockSpec(memory_space=pltpu.VMEM),) * 3,
        cost_estimate=pl.CostEstimate(
            flops=2000 * length * PAIR * PAIR * pairs, bytes_accessed=8 * length * width, transcendentals=0
        ),
    )(queries, keys, values, beta_pre, decay_pre)


def finish_kernel(size, every_ref, local_ref, reach_ref, gates_ref, gain_ref, out_ref):
    _, width = local_ref.shape
    pairs = width // PAIR
    index = lax.axis_index("sp")
    row_ids, col_ids = iotas(PAIR, PAIR)
    same = row_ids // HEAD_DIM == col_ids // HEAD_DIM
    same_half = same.astype(jnp.bfloat16)

    def hop(step, before):
        reached = step < index
        after = []
        for pair in range(pairs):
            item = every_ref[step, pair]
            trans = jnp.where(same, item, jnp.zeros_like(item))
            offset = jnp.where(same, 0.0, item.astype(jnp.float32))
            high = before[pair].astype(jnp.bfloat16)
            low = (before[pair] - high.astype(jnp.float32)).astype(jnp.bfloat16)
            new = offset + dot(trans, high, NN) + dot(trans, low, NN)
            after.append(jnp.where(reached, new, before[pair]))
        return tuple(after)

    start = tuple(jnp.zeros((PAIR, PAIR), jnp.float32) for _ in range(pairs))
    earlier = lax.fori_loop(0, size - 1, hop, start)
    for pair in range(pairs):
        lanes = pl.ds(pair * PAIR, PAIR)
        heads_out = local_ref[:, lanes] + dot(reach_ref[:, lanes], earlier[pair], NN)
        mean = split_dot(heads_out * heads_out, same_half, NN) * (1.0 / HEAD_DIM)
        heads_out = heads_out * lax.rsqrt(mean + EPSILON) * gain_ref[...]
        gated = heads_out * silu(gates_ref[:, lanes].astype(jnp.float32))
        out_ref[:, lanes] = gated.astype(jnp.bfloat16)


def finish(every, local, reach, gates, out_gain):
    length, width = local.shape
    return pl.pallas_call(
        functools.partial(finish_kernel, every.shape[0]),
        name="finish",
        out_shape=jax.ShapeDtypeStruct((length, width), jnp.bfloat16),
        in_specs=[pl.BlockSpec(memory_space=pltpu.VMEM)] * 5,
        out_specs=pl.BlockSpec(memory_space=pltpu.VMEM),
        cost_estimate=pl.CostEstimate(
            flops=4 * length * width * PAIR, bytes_accessed=8 * length * width, transcendentals=0
        ),
    )(every, local, reach, gates, jnp.concatenate([out_gain, out_gain])[None, :])


def exchange_gather(part, axis):
    size = lax.axis_size(axis)
    pieces = {0: part}
    bits = [1 << i for i in range(1, size.bit_length() - 1)] + [1]
    for bit in bits:
        pairs = [(i, i ^ bit) for i in range(size)]
        for held in list(pieces):
            pieces[held ^ bit] = lax.ppermute(pieces[held], axis, pairs)
    return [pieces[m] for m in range(size)]


def place_kernel(middle_ref, sums_ref, out_ref):
    size, index = lax.axis_size("sp"), lax.axis_index("sp")
    width = out_ref.shape[1] // size
    for owner in range(size):
        lanes = pl.ds(owner * width, width)
        start = (index ^ owner) * width
        if width % 128 == 0:
            start = pl.multiple_of(start, 128)
        block = sums_ref[:, pl.ds(start, width)].astype(jnp.float32)
        out_ref[:, lanes] = (middle_ref[:, lanes].astype(jnp.float32) + 0.5 * block).astype(
            jnp.bfloat16
        )


def place(middle, sums):
    return pl.pallas_call(
        place_kernel,
        name="place",
        out_shape=jax.ShapeDtypeStruct(middle.shape, jnp.bfloat16),
        in_specs=[pl.BlockSpec(memory_space=pltpu.VMEM)] * 2,
        out_specs=pl.BlockSpec(memory_space=pltpu.VMEM),
    )(middle, sums)


def layer(
    queries,
    keys,
    values,
    gates,
    decay_pre,
    beta_pre,
    out_gain,
    w_out,
    stream,
    norm_gain,
    w_gate,
    w_up,
    w_down,
):
    n_tp, tp = lax.axis_size("tp"), lax.axis_index("tp")
    gate_whole = lax.all_gather(w_gate, "sp", axis=0, tiled=True)
    up_whole = lax.all_gather(w_up, "sp", axis=0, tiled=True)
    outs = [w_out]
    for shift in range(1, n_tp):
        ring = [(i, (i + shift) % n_tp) for i in range(n_tp)]
        outs.append(lax.ppermute(w_out, "tp", ring))
    downs = exchange_gather(w_down, "sp")

    state, local, reach = mixer(queries, keys, values, beta_pre, decay_pre)
    parts = 2
    step = state.shape[0] // parts
    every = jnp.concatenate(
        [lax.all_gather(state[i * step : (i + 1) * step], "sp") for i in range(parts)], axis=1
    )
    mixed_heads = finish(every, local, reach, gates, out_gain)
    rows = stream.shape[0]
    head_block = lax.all_to_all(
        mixed_heads.reshape(n_tp, rows, mixed_heads.shape[1]), "tp", split_axis=0, concat_axis=0
    )
    projected = 0.0
    for shift in range(n_tp):
        owner = lax.rem(tp + n_tp - shift, n_tp)
        block = lax.dynamic_index_in_dim(head_block, owner, axis=0, keepdims=False)
        projected = projected + jnp.dot(block, outs[shift], preferred_element_type=jnp.float32)
    middle = (stream.astype(jnp.float32) + projected).astype(jnp.bfloat16)
    middle_f = middle.astype(jnp.float32)
    normed = middle_f * lax.rsqrt(jnp.mean(middle_f * middle_f, axis=-1, keepdims=True) + EPSILON)
    normed = (normed * norm_gain).astype(jnp.bfloat16)
    span_rows = jnp.zeros((n_tp * rows, normed.shape[1]), normed.dtype)
    span_rows = lax.dynamic_update_slice_in_dim(span_rows, normed, tp * rows, axis=0)
    for shift in range(1, n_tp):
        ring = [(i, (i + shift) % n_tp) for i in range(n_tp)]
        moved = lax.ppermute(normed, "tp", ring)
        owner = lax.rem(tp + n_tp - shift, n_tp)
        span_rows = lax.dynamic_update_slice_in_dim(span_rows, moved, owner * rows, axis=0)
    gate_hidden = jnp.dot(span_rows, gate_whole, preferred_element_type=jnp.float32)
    up_hidden = jnp.dot(span_rows, up_whole, preferred_element_type=jnp.float32)
    hidden = (jax.nn.silu(gate_hidden) * up_hidden).astype(jnp.bfloat16)
    channel_term = jnp.concatenate(
        [
            jnp.dot(hidden, part, preferred_element_type=jnp.float32).astype(jnp.bfloat16)
            for part in downs
        ],
        axis=1,
    )
    channel_sum = lax.psum_scatter(channel_term, "tp", scatter_dimension=0, tiled=True)
    if w_down.shape[1] % 128 == 0:
        return place(middle, channel_sum)
    size, index = lax.axis_size("sp"), lax.axis_index("sp")
    width = w_down.shape[1]
    blocks = [
        lax.dynamic_slice_in_dim(channel_sum, (index ^ owner) * width, width, axis=1)
        for owner in range(size)
    ]
    channel_sum = jnp.concatenate(blocks, axis=1).astype(jnp.float32)
    return (middle_f + 0.5 * channel_sum).astype(jnp.bfloat16)


def solution(mesh):
    return jax.shard_map(
        layer,
        mesh=mesh,
        in_specs=(
            P("sp", "tp"),
            P("sp", "tp"),
            P("sp", "tp"),
            P("sp", "tp"),
            P("tp", "sp"),
            P("tp", "sp"),
            P(),
            P("tp", None),
            P(("sp", "tp"), None),
            P(),
            P("sp", "tp"),
            P("sp", "tp"),
            P("tp", "sp"),
        ),
        out_specs=P(("sp", "tp"), None),
        check_vma=False,
    )
```
